32 devices in a mesh: rep: 2 (over y), fs: 4 (over z), tp: 4 (over x, core).
Axes of the slice: x: 2, y: 2, z: 4, core: 2. Of those that a mesh axis runs over, the one named last changes fastest.
Arguments:
- tokens: bfloat16 [8, 512, 2048], P(('rep', 'fs')), may hold values from -6 to 6
- first_gain: float32 [2048], replicated, may hold values from 0.1 to 1.9
- in_matrix: float32 [2048, 2048], P('fs', 'tp'), may hold values from -0.125 to 0.125
- in_scale: float32 [2048], P('tp'), may hold values from 0.5 to 2
- conv_taps: float32 [4, 2048], P(None, 'tp'), may hold values from -3 to 3
- decay_rate: float32 [2, 2048], P(None, 'tp'), may hold values from 0 to 1, as said below
- recall_maps: float32 [2, 8, 256, 256], P(None, 'tp'), may hold values from -0.375 to 0.375
- admit_maps: float32 [2, 8, 256, 256], P(None, 'tp'), may hold values from -0.375 to 0.375
- out_matrix: float32 [2048, 2048], P('fs', 'tp'), may hold values from -0.125 to 0.125
- out_scale: float32 [2048], P('fs'), may hold values from 0.5 to 2
- second_gain: float32 [2048], replicated, may hold values from 0.1 to 1.9
- up_matrix: float32 [2048, 4096], P('fs', 'tp'), may hold values from -0.125 to 0.125
- up_scale: float32 [4096], P('tp'), may hold values from 0.5 to 2
- down_matrix: float32 [2048, 4096], P('fs', 'tp'), may hold values from -0.09375 to 0.09375
- down_scale: float32 [2048], P('fs'), may hold values from 0.5 to 2
Outputs:
- layer_out: bfloat16 [8, 512, 2048], P(('rep', 'fs'))
The draws below stay inside these ranges and needn't reach their ends.
Inputs may be any that keep to these rules, and one draw needn't show every extreme that they name: `decay_rate`: positive per-step decay rates.
All inputs are finite; a program needn't handle non-finite values.
Results may differ from the reference program's by a relative error of at most 0.024.
Values may be sent and summed in bfloat16 or wider, within the bound.
A program may use at most 64 MiB of HBM per device.

```python
import math
import jax
import jax.numpy as jnp
from jax import lax

D = 2048
BLOCK = 256
BLOCKS = 8
FF = 4096
TAPS = 4
LEN = 512
REC_WIDTH = 2048
SEQS = 8
N_TP = 4


def draw_decay_rate(key, part):
    pick_key, slow_key, fast_key = jax.random.split(jax.random.fold_in(key, 17), 3)
    shape = (2, REC_WIDTH)
    slow_share = 0.5
    slow_pick = jax.random.bernoulli(pick_key, slow_share, shape)
    slow_rate = jnp.exp(jax.random.uniform(slow_key, shape, jnp.float32, math.log(0.05), math.log(0.5))) / LEN
    fast_rate = jnp.exp(jax.random.uniform(fast_key, shape, jnp.float32, math.log(0.005), math.log(0.02)))
    return jnp.where(slow_pick, slow_rate, fast_rate).astype(jnp.float32)


def level_of(key, extent, cuts, least, top_value):
    factor_of, own = 1.0, jax.random.fold_in(key, 6)
    for dim, blocks in cuts:
        heights = jnp.exp(jax.random.uniform(jax.random.fold_in(own, dim), (blocks,), jnp.float32, least / len(cuts), top_value / len(cuts)))
        factor_of = factor_of * jnp.repeat(heights, extent[dim] // blocks).reshape([-1 if axis == dim else 1 for axis in range(len(extent))])
    return factor_of


def bell_draw(rng, dims, deviation, reach, pieces=(), dtype=jnp.bfloat16):
    level = level_of(rng, dims, pieces, -0.22, 0.18) if pieces else 1.0
    entries = jax.random.normal(rng, dims, jnp.float32) * deviation * level
    return jnp.minimum(jnp.maximum(entries, -reach), reach).astype(dtype)


def setup_inputs(seed: int = 0) -> dict:
    seeds = jax.random.split(jax.random.key(seed), 16)
    return {
        "tokens": bell_draw(seeds[0], (SEQS, LEN, D), 1.0, 6.0, ((0, 8),)),
        "first_gain": jnp.clip(1.0 + 0.18 * jax.random.normal(seeds[1], (D,), jnp.float32), 0.1, 1.9),
        "in_matrix": bell_draw(seeds[2], (D, REC_WIDTH), D ** -0.5, 0.125, ((0, 4), (1, 4)), jnp.float32),
        "in_scale": jnp.clip(jnp.exp(math.log(2.0) - 1.3862944 * jax.random.uniform(seeds[3], (REC_WIDTH,), jnp.float32) ** level_of(seeds[3], (REC_WIDTH,), ((0, 4),), -0.2, 0.2)), 0.5, 2.0),
        "conv_taps": bell_draw(seeds[4], (TAPS, REC_WIDTH), TAPS ** -0.5, 3.0, ((1, 4),), jnp.float32),
        "decay_rate": draw_decay_rate(jax.random.fold_in(seeds[15], 71), 0),
        "recall_maps": bell_draw(seeds[6], (2, BLOCKS, BLOCK, BLOCK), BLOCK ** -0.5, 0.375, ((1, 4),), jnp.float32),
        "admit_maps": bell_draw(seeds[7], (2, BLOCKS, BLOCK, BLOCK), BLOCK ** -0.5, 0.375, ((1, 4),), jnp.float32),
        "out_matrix": bell_draw(seeds[8], (D, REC_WIDTH), REC_WIDTH ** -0.5, 0.125, ((0, 4), (1, 4)), jnp.float32),
        "out_scale": jnp.clip(jnp.exp(math.log(2.0) - 1.3862944 * jax.random.uniform(seeds[9], (D,), jnp.float32) ** level_of(seeds[9], (D,), ((0, 4),), -0.2, 0.2)), 0.5, 2.0),
        "second_gain": jnp.clip(1.0 + 0.18 * jax.random.normal(seeds[10], (D,), jnp.float32), 0.1, 1.9),
        "up_matrix": bell_draw(seeds[11], (D, FF), D ** -0.5, 0.125, ((0, 4), (1, 4)), jnp.float32),
        "up_scale": jnp.clip(jnp.exp(math.log(2.0) - 1.3862944 * jax.random.uniform(seeds[12], (FF,), jnp.float32) ** level_of(seeds[12], (FF,), ((0, 4),), -0.2, 0.2)), 0.5, 2.0),
        "down_matrix": bell_draw(seeds[13], (D, FF), FF ** -0.5, 0.09375, ((0, 4), (1, 4)), jnp.float32),
        "down_scale": jnp.clip(jnp.exp(math.log(2.0) - 1.3862944 * jax.random.uniform(seeds[14], (D,), jnp.float32) ** level_of(seeds[14], (D,), ((0, 4),), -0.2, 0.2)), 0.5, 2.0),
    }


EPSILON = 1e-06
RATE_GAIN = 8.0

def normalize(stream, gain):
    return stream * lax.rsqrt(lax.optimization_barrier(jnp.mean(stream * stream, axis=-1, keepdims=True)) + EPSILON) * gain

def convolve(values, taps):
    length = values.shape[0]
    count = taps.shape[0]
    padded = jnp.pad(values, ((count // 2, count - 1 - count // 2), (0, 0)))
    total = taps[0] * padded[0:length]
    for offset in range(1, count):
        total = total + taps[offset] * padded[offset:offset + length]
    return total

def block_map(values, maps):
    length = values.shape[0]
    count, width = (maps.shape[0], maps.shape[1])
    grouped = values.reshape(length, count, width)
    mapped = jnp.einsum('lnj,njk->lnk', grouped, maps, precision=lax.Precision.HIGHEST)
    return mapped.reshape(length, count * width)

def combine_steps(earlier, later):
    return (earlier[0] * later[0], later[0] * earlier[1] + later[1])

def one_direction(values, rate, recall_map, admit_map):
    recall = jax.nn.sigmoid(block_map(values, recall_map))
    admit = jax.nn.sigmoid(block_map(values, admit_map))
    log_decay = -RATE_GAIN * recall * rate
    decay = jnp.exp(log_decay)
    drive = jnp.sqrt(-jnp.expm1(2.0 * log_decay)) * admit * values
    carried = lax.associative_scan(combine_steps, (decay, drive), axis=0)
    return carried[1]

def recurrence(values, rates, recall_maps, admit_maps):
    forward = one_direction(values, rates[0], recall_maps[0], admit_maps[0])
    backward = one_direction(values[::-1], rates[1], recall_maps[1], admit_maps[1])[::-1]
    return forward + backward

def block_sum(values, matrix):
    length, width = values.shape
    model = matrix.shape[0]
    split_values = values.astype(jnp.float32).reshape(length, N_TP, width // N_TP)
    split_matrix = matrix.astype(jnp.float32).reshape(model, N_TP, width // N_TP)
    parts = jnp.einsum('lte,dte->tld', split_values, split_matrix, precision=lax.Precision.HIGHEST)
    rounded = lax.optimization_barrier(parts.astype(jnp.bfloat16))
    return lax.optimization_barrier(jnp.sum(rounded.astype(jnp.float32), axis=0))

def reference(tokens, first_gain, in_matrix, in_scale, conv_taps, decay_rate, recall_maps, admit_maps, out_matrix, out_scale, second_gain, up_matrix, up_scale, down_matrix, down_scale):
    in_cols = in_matrix.astype(jnp.bfloat16)
    out_rows = out_matrix.astype(jnp.bfloat16)
    up_cols = up_matrix.astype(jnp.bfloat16)
    down_rows = down_matrix.astype(jnp.bfloat16)
    in_factor = in_scale.astype(jnp.bfloat16)
    out_factor = out_scale.astype(jnp.bfloat16)
    up_factor = up_scale.astype(jnp.bfloat16)
    down_factor = down_scale.astype(jnp.bfloat16)

    def one_sequence(sequence):
        stream = sequence.astype(jnp.float32)
        normed = normalize(stream, first_gain).astype(jnp.bfloat16)
        before = (jnp.dot(normed, in_cols, preferred_element_type=jnp.float32) * in_factor).astype(jnp.bfloat16)
        conv_out = convolve(before.astype(jnp.float32), conv_taps)
        mixed = recurrence(conv_out, decay_rate, recall_maps, admit_maps).astype(jnp.bfloat16)
        middle = stream + out_factor * block_sum(mixed, out_rows)
        second_normed = normalize(middle, second_gain).astype(jnp.bfloat16)
        raised = jnp.dot(second_normed, up_cols, preferred_element_type=jnp.float32) * up_factor
        active = jnp.square(jax.nn.relu(raised)).astype(jnp.bfloat16)
        return (middle + down_factor * block_sum(active, down_rows)).astype(jnp.bfloat16)
    return lax.map(one_sequence, tokens)
```

```python
import functools
import jax
import jax.numpy as jnp
from jax import lax
from jax.experimental import pallas as pl
from jax.experimental.pallas import tpu as pltpu
from jax.sharding import PartitionSpec as P

EPSILON = 1e-06
RATE_GAIN = 8.0
LANES = 128
SEGMENTS = 8
PAD = 8


def normalize(stream, gain):
    return stream * lax.rsqrt(jnp.mean(stream * stream, axis=-1, keepdims=True) + EPSILON) * gain


def one_minus_exp(y):
    series = 1.0 + y * (1.0 / 6.0)
    for k in (5.0, 4.0, 3.0, 2.0):
        series = 1.0 + y * (1.0 / k) * series
    return jnp.where(y > -0.25, -y * series, 1.0 - jnp.exp(y))


def sigmoid(x):
    return 0.5 * jnp.tanh(0.5 * x) + 0.5


def recurrence_kernel(before_ref, taps_ref, rate_ref, recall_ref, admit_ref, mixed_ref, padded, decay, drive, prefix):
    length, width = before_ref.shape
    directions, groups, block, _ = recall_ref.shape
    taps = taps_ref.shape[0]
    chunks = width // LANES
    steps = length // SEGMENTS

    edge = jnp.zeros((PAD, width), jnp.float32)
    padded[pl.ds(0, PAD), :] = edge
    padded[pl.ds(PAD + length, PAD), :] = edge
    padded[pl.ds(PAD, length), :] = before_ref[...].astype(jnp.float32)

    rows = length // SEGMENTS
    weights = [
        [(recall_ref[d, g].astype(jnp.bfloat16), admit_ref[d, g].astype(jnp.bfloat16)) for g in range(groups)]
        for d in range(directions)
    ]

    for tile in range(SEGMENTS):
        base = tile * rows
        conv = taps_ref[0:1, :] * padded[pl.ds(base + PAD - taps // 2, rows), :]
        for k in range(1, taps):
            conv = conv + taps_ref[k : k + 1, :] * padded[pl.ds(base + PAD - taps // 2 + k, rows), :]
        narrow = conv.astype(jnp.bfloat16)
        for g in range(groups):
            values = conv[:, g * block : (g + 1) * block]
            left = narrow[:, g * block : (g + 1) * block]
            for d in range(directions):
                recall_map, admit_map = weights[d][g]
                recall = sigmoid(jnp.dot(left, recall_map, preferred_element_type=jnp.float32))
                admit = sigmoid(jnp.dot(left, admit_map, preferred_element_type=jnp.float32))
                log_decay = recall * (-RATE_GAIN * rate_ref[d : d + 1, g * block : (g + 1) * block])
                a = jnp.exp(log_decay)
                b = jnp.sqrt(one_minus_exp(2.0 * log_decay)) * admit * values
                for c in range(block // LANES):
                    where = g * (block // LANES) + c
                    decay[d, where, pl.ds(base, rows), :] = a[:, c * LANES : (c + 1) * LANES]
                    drive[d, where, pl.ds(base, rows), :] = b[:, c * LANES : (c + 1) * LANES]

    lanes = [(d, c) for d in range(directions) for c in range(chunks)]

    def scan_step(s, carried):
        out = []
        for (d, c), (state, product) in zip(lanes, carried):
            at = s if d == 0 else steps - 1 - s
            a = decay[d, c, pl.ds(at, SEGMENTS, stride=steps), :]
            b = drive[d, c, pl.ds(at, SEGMENTS, stride=steps), :]
            state = a * state + b
            product = a * product
            drive[d, c, pl.ds(at, SEGMENTS, stride=steps), :] = state
            prefix[d, c, pl.ds(at, SEGMENTS, stride=steps), :] = product
            out.append((state, product))
        return tuple(out)

    start = tuple((jnp.zeros((SEGMENTS, LANES), jnp.float32), jnp.ones((SEGMENTS, LANES), jnp.float32)) for _ in lanes)
    ends = lax.fori_loop(0, steps, scan_step, start, unroll=4)
    ends = dict(zip(lanes, ends))

    for c in range(chunks):
        carries = []
        for d in range(directions):
            state, product = ends[(d, c)]
            order = range(SEGMENTS) if d == 0 else range(SEGMENTS - 1, -1, -1)
            carry = jnp.zeros((1, LANES), jnp.float32)
            entering = {}
            for k in order:
                entering[k] = carry
                carry = product[k : k + 1, :] * carry + state[k : k + 1, :]
            carries.append(entering)
        for k in range(SEGMENTS):
            span = pl.ds(k * steps, steps)
            total = drive[0, c, span, :] + prefix[0, c, span, :] * carries[0][k]
            total = total + (drive[1, c, span, :] + prefix[1, c, span, :] * carries[1][k])
            mixed_ref[span, c * LANES : (c + 1) * LANES] = total.astype(jnp.bfloat16)


def recurrence(before, taps, rates, recall_maps, admit_maps):
    length, width = before.shape
    directions = rates.shape[0]
    chunks = width // LANES
    plane = pltpu.VMEM((directions, chunks, length, LANES), jnp.float32)
    return pl.pallas_call(
        recurrence_kernel,
        out_shape=jax.ShapeDtypeStruct((length, width), jnp.bfloat16),
        in_specs=[pl.BlockSpec(memory_space=pltpu.VMEM)] * 5,
        out_specs=pl.BlockSpec(memory_space=pltpu.VMEM),
        scratch_shapes=[pltpu.VMEM((length + 2 * PAD, width), jnp.float32), plane, plane, plane],
        compiler_params=pltpu.CompilerParams(vmem_limit_bytes=24 * 2**20),
        cost_estimate=pl.CostEstimate(flops=16 * length * width * 256, bytes_accessed=8 * 2**20, transcendentals=8 * length * width),
        name="recurrence",
    )(before, taps, rates, recall_maps, admit_maps)


def contract_last(left, right):
    return lax.dot_general(
        left, right, (((1,), (1,)), ((), ())), preferred_element_type=jnp.float32
    )


def gather(shard):
    copies = lax.axis_size("rep")
    if shard.shape[0] % (16 * copies):
        return lax.all_gather(shard.astype(jnp.bfloat16), "fs", axis=0, tiled=True)
    rows = shard.shape[0] // copies
    part = lax.dynamic_slice_in_dim(shard, lax.axis_index("rep") * rows, rows, 0)
    return lax.all_gather(part.astype(jnp.bfloat16), ("fs", "rep"), axis=0, tiled=True)


def body(
    tokens,
    first_gain,
    in_matrix,
    in_scale,
    conv_taps,
    decay_rate,
    recall_maps,
    admit_maps,
    out_matrix,
    out_scale,
    second_gain,
    up_matrix,
    up_scale,
    down_matrix,
    down_scale,
):
    stream = tokens.reshape(tokens.shape[1], tokens.shape[2]).astype(jnp.float32)
    factors = lax.all_gather(
        jnp.stack([out_scale, down_scale]).astype(jnp.bfloat16), "fs", axis=1, tiled=True
    )
    in_cols = gather(in_matrix)
    normed = normalize(stream, first_gain).astype(jnp.bfloat16)
    before = (
        jnp.dot(normed, in_cols, preferred_element_type=jnp.float32) * in_scale.astype(jnp.bfloat16)
    ).astype(jnp.bfloat16)
    mixed = recurrence(before, conv_taps, decay_rate, recall_maps, admit_maps)
    partial_value = contract_last(mixed, gather(out_matrix))
    middle = stream + factors[0] * lax.psum(partial_value.astype(jnp.bfloat16), "tp").astype(
        jnp.float32
    )
    second_normed = normalize(middle, second_gain).astype(jnp.bfloat16)
    raised = jnp.dot(second_normed, gather(up_matrix), preferred_element_type=jnp.float32)
    active = jnp.square(jax.nn.relu(raised * up_scale.astype(jnp.bfloat16))).astype(jnp.bfloat16)
    lowered = contract_last(active, gather(down_matrix))
    result = (
        middle + factors[1] * lax.psum(lowered.astype(jnp.bfloat16), "tp").astype(jnp.float32)
    ).astype(jnp.bfloat16)
    return result.reshape(tokens.shape)


def solution(mesh):
    placed = (
        P(("rep", "fs"), None, None),
        P(),
        P("fs", "tp"),
        P("tp"),
        P(None, "tp"),
        P(None, "tp"),
        P(None, "tp", None, None),
        P(None, "tp", None, None),
        P("fs", "tp"),
        P("fs"),
        P(),
        P("fs", "tp"),
        P("tp"),
        P("fs", "tp"),
        P("fs"),
    )
    return jax.shard_map(
        body, mesh=mesh, in_specs=placed, out_specs=P(("rep", "fs"), None, None), check_vma=False
    )
```

```python
import functools
import jax
import jax.numpy as jnp
from jax import lax
from jax.experimental import pallas as pl
from jax.experimental.pallas import tpu as pltpu
from jax.sharding import PartitionSpec as P

EPSILON = 1e-06
RATE_GAIN = 8.0
LANES = 128
SEGMENTS = 8
PAD = 8


def normalize(stream, gain):
    return stream * lax.rsqrt(jnp.mean(stream * stream, axis=-1, keepdims=True) + EPSILON) * gain


def one_minus_exp(y):
    series = 1.0 + y * (1.0 / 6.0)
    for k in (5.0, 4.0, 3.0, 2.0):
        series = 1.0 + y * (1.0 / k) * series
    return jnp.where(y > -0.25, -y * series, 1.0 - jnp.exp(y))


def sigmoid(x):
    return 0.5 * jnp.tanh(0.5 * x) + 0.5


def gate_part(padded, taps_ref, rate_ref, recall_ref, admit_ref, decay, drive, length):
    directions, groups, block, _ = recall_ref.shape
    taps = taps_ref.shape[0]
    rows = length // SEGMENTS

    def tile_step(tile, _):
        base = pl.multiple_of(tile * rows, rows)
        conv = jnp.zeros((rows, padded.shape[1]), jnp.float32)
        window = padded[pl.ds(base, rows + 2 * PAD), :]
        for k in range(taps):
            first = PAD - taps // 2 + k
            conv = conv + taps_ref[k : k + 1, :] * window[first : first + rows, :]
        narrow = conv.astype(jnp.bfloat16)
        for g in range(groups):
            values = conv[:, g * block : (g + 1) * block]
            left = narrow[:, g * block : (g + 1) * block]
            for d in range(directions):
                recall = sigmoid(jnp.dot(left, recall_ref[d, g].astype(jnp.bfloat16), preferred_element_type=jnp.float32))
                admit = sigmoid(jnp.dot(left, admit_ref[d, g].astype(jnp.bfloat16), preferred_element_type=jnp.float32))
                log_decay = recall * (-RATE_GAIN * rate_ref[d : d + 1, g * block : (g + 1) * block])
                a = jnp.exp(log_decay)
                b = jnp.sqrt(one_minus_exp(2.0 * log_decay)) * admit * values
                for c in range(block // LANES):
                    where = g * (block // LANES) + c
                    decay[d, where, pl.ds(base, rows), :] = a[:, c * LANES : (c + 1) * LANES]
                    drive[d, where, pl.ds(base, rows), :] = b[:, c * LANES : (c + 1) * LANES]
        return 0

    lax.fori_loop(0, SEGMENTS, tile_step, 0)


def scan_part(decay, drive, prefix, mixed_ref, length):
    directions, chunks = decay.shape[:2]
    steps = length // SEGMENTS
    lanes = [(d, c) for d in range(directions) for c in range(chunks)]

    def scan_step(s, carried):
        out = []
        for (d, c), (state, product) in zip(lanes, carried):
            at = s if d == 0 else steps - 1 - s
            a = decay[d, c, pl.ds(at, SEGMENTS, stride=steps), :]
            b = drive[d, c, pl.ds(at, SEGMENTS, stride=steps), :]
            state = a * state + b
            product = a * product
            drive[d, c, pl.ds(at, SEGMENTS, stride=steps), :] = state
            prefix[d, c, pl.ds(at, SEGMENTS, stride=steps), :] = product
            out.append((state, product))
        return tuple(out)

    start = tuple((jnp.zeros((SEGMENTS, LANES), jnp.float32), jnp.ones((SEGMENTS, LANES), jnp.float32)) for _ in lanes)
    ends = lax.fori_loop(0, steps, scan_step, start, unroll=4)
    ends = dict(zip(lanes, ends))

    for c in range(chunks):
        carries = []
        for d in range(directions):
            state, product = ends[(d, c)]
            order = range(SEGMENTS) if d == 0 else range(SEGMENTS - 1, -1, -1)
            carry = jnp.zeros((1, LANES), jnp.float32)
            entering = {}
            for k in order:
                entering[k] = carry
                carry = product[k : k + 1, :] * carry + state[k : k + 1, :]
            carries.append(entering)
        for k in range(SEGMENTS):
            span = pl.ds(k * steps, steps)
            total = drive[0, c, span, :] + prefix[0, c, span, :] * carries[0][k]
            total = total + (drive[1, c, span, :] + prefix[1, c, span, :] * carries[1][k])
            mixed_ref[span, c * LANES : (c + 1) * LANES] = total.astype(jnp.bfloat16)


def recurrence_kernel(before_ref, taps_ref, rate_ref, recall_ref, admit_ref, mixed_ref, padded, decay, drive, prefix):
    length, width = before_ref.shape
    edge = jnp.zeros((PAD, width), jnp.float32)
    padded[pl.ds(0, PAD), :] = edge
    padded[pl.ds(PAD + length, PAD), :] = edge
    padded[pl.ds(PAD, length), :] = before_ref[...].astype(jnp.float32)
    gate_part(padded, taps_ref, rate_ref, recall_ref, admit_ref, decay, drive, length)
    scan_part(decay, drive, prefix, mixed_ref, length)


def recurrence(before, taps, rates, recall_maps, admit_maps):
    length, width = before.shape
    directions = rates.shape[0]
    chunks = width // LANES
    plane = pltpu.VMEM((directions, chunks, length, LANES), jnp.float32)
    return pl.pallas_call(
        recurrence_kernel,
        out_shape=jax.ShapeDtypeStruct((length, width), jnp.bfloat16),
        in_specs=[pl.BlockSpec(memory_space=pltpu.VMEM)] * 5,
        out_specs=pl.BlockSpec(memory_space=pltpu.VMEM),
        scratch_shapes=[pltpu.VMEM((length + 2 * PAD, width), jnp.float32), plane, plane, plane],
        compiler_params=pltpu.CompilerParams(vmem_limit_bytes=24 * 2**20),
        cost_estimate=pl.CostEstimate(flops=16 * length * width * 256, bytes_accessed=8 * 2**20, transcendentals=8 * length * width),
        name="recurrence",
    )(before, taps, rates, recall_maps, admit_maps)


def contract_last(left, right):
    return lax.dot_general(
        left, right, (((1,), (1,)), ((), ())), preferred_element_type=jnp.float32
    )


def gather(shard):
    copies = lax.axis_size("rep")
    if shard.shape[0] % (16 * copies):
        return lax.all_gather(shard.astype(jnp.bfloat16), "fs", axis=0, tiled=True)
    rows = shard.shape[0] // copies
    part = lax.dynamic_slice_in_dim(shard, lax.axis_index("rep") * rows, rows, 0)
    return lax.all_gather(part.astype(jnp.bfloat16), ("fs", "rep"), axis=0, tiled=True)


def body(
    tokens,
    first_gain,
    in_matrix,
    in_scale,
    conv_taps,
    decay_rate,
    recall_maps,
    admit_maps,
    out_matrix,
    out_scale,
    second_gain,
    up_matrix,
    up_scale,
    down_matrix,
    down_scale,
):
    stream = tokens.reshape(tokens.shape[1], tokens.shape[2]).astype(jnp.float32)
    factors = lax.all_gather(
        jnp.stack([out_scale, down_scale]).astype(jnp.bfloat16), "fs", axis=1, tiled=True
    )
    in_cols = gather(in_matrix)
    normed = normalize(stream, first_gain).astype(jnp.bfloat16)
    before = (
        jnp.dot(normed, in_cols, preferred_element_type=jnp.float32) * in_scale.astype(jnp.bfloat16)
    ).astype(jnp.bfloat16)
    mixed = recurrence(before, conv_taps, decay_rate, recall_maps, admit_maps)
    partial_value = contract_last(mixed, gather(out_matrix))
    middle = stream + factors[0] * lax.psum(partial_value.astype(jnp.bfloat16), "tp").astype(
        jnp.float32
    )
    second_normed = normalize(middle, second_gain).astype(jnp.bfloat16)
    raised = jnp.dot(second_normed, gather(up_matrix), preferred_element_type=jnp.float32)
    active = jnp.square(jax.nn.relu(raised * up_scale.astype(jnp.bfloat16))).astype(jnp.bfloat16)
    lowered = contract_last(active, gather(down_matrix))
    result = (
        middle + factors[1] * lax.psum(lowered.astype(jnp.bfloat16), "tp").astype(jnp.float32)
    ).astype(jnp.bfloat16)
    return result.reshape(tokens.shape)

MESH = pl.DeviceIdType.MESH


def layer_kernel(
    names, tokens_ref, first_ref, in_ref, in_scale_ref, taps_ref, rate_ref, recall_ref, admit_ref,
    out_ref, second_ref, up_ref, up_scale_ref, down_ref, scales_ref,
    result_ref,
    in_all, out_all, up_all, down_all, scales_all, normed, padded, decay, drive, prefix, mixed, active,
    first_parts, first_sums, second_parts, second_sums, middle, send, recv,
):
    replica, place, rank = (lax.axis_index(name) for name in names)
    rep_name, fs_name, tp_name = names
    fs, tp = 4, 4
    length, model = tokens_ref.shape
    rows = length // tp
    block = model // fs
    right, left, across = (lax.rem(place + k, fs) for k in (1, 3, 2))
    mate = 1 - replica
    near = rank + 1 - 2 * lax.rem(rank, 2)
    far = lax.rem(rank + 2, tp)
    count = [0]

    def copy(src, dst, axis, peer):
        index = count[0]
        count[0] += 1
        return pltpu.make_async_remote_copy(
            src_ref=src, dst_ref=dst, send_sem=send.at[index], recv_sem=recv.at[index],
            device_id={axis: peer}, device_id_type=MESH,
        )

    started = []

    def start(*copies):
        for one in copies:
            one.start()
            started.append(one)

    class Gather:
        def __init__(self, whole):
            def view(owner, offset, size):
                return whole.at[pl.ds(pl.multiple_of(owner * block + replica * half + offset, quarter), size), :]

            half, quarter = block // 2, block // 4
            own = view(place, 0, half)
            from_left, from_right = view(left, 0, half), view(right, 0, half)
            self.to_right = copy(own, own, fs_name, right)
            self.to_left = copy(own, own, fs_name, left)
            low, high = view(left, 0, quarter), view(right, quarter, quarter)
            self.on_right = copy(low, low, fs_name, right)
            self.on_left = copy(high, high, fs_name, left)
            opposite = view(across, 0, half)
            self.swaps = [copy(part, part, rep_name, mate) for part in (from_left, from_right, opposite)]

        def first(self):
            start(self.to_right, self.to_left)

        def second(self):
            self.to_right.wait_recv()
            start(self.on_right, self.swaps[0])
            self.to_left.wait_recv()
            start(self.on_left, self.swaps[1])

        def third(self):
            self.on_right.wait_recv()
            self.on_left.wait_recv()
            start(self.swaps[2])

        def finish(self):
            for swap in self.swaps:
                swap.wait_recv()

    barrier = pltpu.get_barrier_semaphore()
    greeted = [(rep_name, mate), (fs_name, right), (fs_name, left), (fs_name, across)]
    greeted += [(tp_name, lax.rem(rank + k, tp)) for k in range(1, tp)]
    for axis, peer in greeted:
        pl.semaphore_signal(barrier, inc=1, device_id={axis: peer}, device_id_type=MESH)

    own_rows = pl.ds(pl.multiple_of(place * block, block), block)
    for shard, whole in ((in_ref, in_all), (out_ref, out_all), (up_ref, up_all), (down_ref, down_all)):
        whole[own_rows, :] = shard[...].astype(jnp.bfloat16)
    scales_all[place] = scales_ref[...]
    pl.semaphore_wait(barrier, len(greeted))

    g_in, g_out, g_up, g_down = (Gather(whole) for whole in (in_all, out_all, up_all, down_all))
    g_in.first()
    scale_copies = [
        copy(scales_ref, scales_all.at[place], fs_name, lax.rem(place + k, fs)) for k in range(1, fs)
    ]
    start(*scale_copies)
    g_out.first()

    tile = 64

    def norm_step(i, _):
        at = pl.ds(pl.multiple_of(i * tile, tile), tile)
        normed[at, :] = normalize(tokens_ref[at, :].astype(jnp.float32), first_ref[...]).astype(jnp.bfloat16)
        return 0

    lax.fori_loop(0, length // tile, norm_step, 0)

    g_in.second()
    g_in.third()
    g_out.second()
    g_up.first()
    g_in.finish()

    edge = jnp.zeros((PAD, padded.shape[1]), jnp.float32)
    padded[pl.ds(0, PAD), :] = edge
    padded[pl.ds(PAD + length, PAD), :] = edge
    wide = 256

    def in_step(i, _):
        at = pl.ds(pl.multiple_of(i * wide, wide), wide)
        product = jnp.dot(normed[...], in_all[:, at], preferred_element_type=jnp.float32)
        product = product * in_scale_ref[:, at].astype(jnp.bfloat16).astype(jnp.float32)
        padded[pl.ds(PAD, length), at] = product.astype(jnp.bfloat16).astype(jnp.float32)
        return 0

    lax.fori_loop(0, in_all.shape[1] // wide, in_step, 0)
    g_out.third()
    gate_part(padded, taps_ref, rate_ref, recall_ref, admit_ref, decay, drive, length)
    g_up.second()
    g_down.first()
    scan_part(decay, drive, prefix, mixed, length)
    g_up.third()
    g_out.finish()
    for one in scale_copies:
        one.wait_recv()

    def project(values, whole, parts, sums, between):
        hops = []

        def send_block(j):
            hop = []
            for k in range(1, tp):
                peer = lax.rem(rank + k, tp)
                hop.append(copy(parts.at[j, pl.ds(pl.multiple_of(peer * rows, rows), rows), :], sums.at[k - 1, j], tp_name, peer))
            start(*hop)
            hops.append(hop)

        for j in range(fs):
            def step(i, _):
                at = pl.ds(pl.multiple_of(i * wide, wide), wide)
                matrix = whole[pl.ds(pl.multiple_of(j * block + i * wide, wide), wide), :]
                parts[j, :, at] = contract_last(values[...], matrix).astype(jnp.bfloat16)
                return 0

            lax.fori_loop(0, block // wide, step, 0)
            if j:
                send_block(j - 1)
            between(j)
        send_block(fs - 1)
        return hops

    own_quarter = pl.ds(pl.multiple_of(rank * rows, rows), rows)

    def summed(parts, sums, hops, j):
        for hop in hops[j]:
            hop.wait_recv()
        total = parts[j, own_quarter, :].astype(jnp.float32)
        for k in range(tp - 1):
            total = total + sums[k, j].astype(jnp.float32)
        return total

    def factor(j, which):
        return scales_all[j, which : which + 1, :].astype(jnp.bfloat16).astype(jnp.float32)

    def advance(j):
        if j == 1:
            g_down.second()

    hops = project(mixed, out_all, first_parts, first_sums, advance)
    squares = jnp.zeros((rows, 1), jnp.float32)
    for j in range(fs):
        columns = slice(j * block, (j + 1) * block)
        value = tokens_ref[own_quarter, columns].astype(jnp.float32) + factor(j, 0) * summed(first_parts, first_sums, hops, j)
        middle[:, columns] = value
        squares = squares + jnp.sum(value * value, axis=1, keepdims=True)
    inverse = lax.rsqrt(squares * (1.0 / model) + EPSILON)
    normed[own_quarter, :] = (middle[...] * inverse * second_ref[...]).astype(jnp.bfloat16)

    def spread(ref, columns):
        own = ref.at[own_quarter, columns]
        theirs = ref.at[pl.ds(pl.multiple_of(far * rows, rows), rows), columns]
        return copy(own, own, tp_name, far), copy(own, own, tp_name, near), copy(theirs, theirs, tp_name, near)

    whole_width = pl.ds(0, model)
    to_far, to_near, onward = spread(normed, whole_width)
    g_up.finish()
    start(to_far, to_near)
    g_down.third()
    to_far.wait_recv()
    start(onward)
    to_near.wait_recv()
    onward.wait_recv()

    def up_step(i, _):
        at = pl.ds(pl.multiple_of(i * wide, wide), wide)
        raised = jnp.dot(normed[...], up_all[:, at], preferred_element_type=jnp.float32)
        raised = raised * up_scale_ref[:, at].astype(jnp.bfloat16).astype(jnp.float32)
        active[:, at] = jnp.square(jnp.maximum(raised, 0.0)).astype(jnp.bfloat16)
        return 0

    lax.fori_loop(0, up_all.shape[1] // wide, up_step, 0)
    g_down.finish()
    hops = project(active, down_all, second_parts, second_sums, lambda j: None)
    spreads = []
    for j in range(fs):
        columns = slice(j * block, (j + 1) * block)
        value = middle[:, columns] + factor(j, 1) * summed(second_parts, second_sums, hops, j)
        result_ref[own_quarter, columns] = value.astype(jnp.bfloat16)
        spreads.append(spread(result_ref, pl.ds(j * block, block)))
        start(*spreads[j][:2])
        if j:
            spreads[j - 1][0].wait_recv()
            start(spreads[j - 1][2])
    spreads[-1][0].wait_recv()
    start(spreads[-1][2])
    for _, to_near, onward in spreads:
        to_near.wait_recv()
        onward.wait_recv()
    for one in started:
        one.wait_send()


def fused_body(
    tokens, first_gain, in_matrix, in_scale, conv_taps, decay_rate, recall_maps, admit_maps,
    out_matrix, out_scale, second_gain, up_matrix, up_scale, down_matrix, down_scale,
):
    length, model = tokens.shape[1:]
    width, hidden = in_matrix.shape[1], up_matrix.shape[1]
    fs, tp = lax.axis_size("fs"), lax.axis_size("tp")
    rows, block = length // tp, model // fs
    directions = decay_rate.shape[0]
    plane = pltpu.VMEM((directions, width // LANES, length, LANES), jnp.float32)
    parts = pltpu.VMEM((fs, length, block), jnp.bfloat16)
    sums = pltpu.VMEM((tp - 1, fs, rows, block), jnp.bfloat16)
    copies = 4 * 7 + 3 + 2 * 12 + 3 + 12
    result = pl.pallas_call(
        functools.partial(layer_kernel, ("rep", "fs", "tp")),
        out_shape=jax.ShapeDtypeStruct((length, model), jnp.bfloat16),
        in_specs=[pl.BlockSpec(memory_space=pltpu.VMEM)] * 14,
        out_specs=pl.BlockSpec(memory_space=pltpu.VMEM),
        scratch_shapes=[
            pltpu.VMEM((model, width), jnp.bfloat16),
            pltpu.VMEM((model, width), jnp.bfloat16),
            pltpu.VMEM((model, hidden), jnp.bfloat16),
            pltpu.VMEM((model, hidden), jnp.bfloat16),
            pltpu.VMEM((fs, 2, block), jnp.float32),
            pltpu.VMEM((length, model), jnp.bfloat16),
            pltpu.VMEM((length + 2 * PAD, width), jnp.float32),
            plane, plane, plane,
            pltpu.VMEM((length, width), jnp.bfloat16),
            pltpu.VMEM((length, hidden), jnp.bfloat16),
            parts, sums, parts, sums,
            pltpu.VMEM((rows, model), jnp.float32),
            pltpu.SemaphoreType.DMA((copies,)),
            pltpu.SemaphoreType.DMA((copies,)),
        ],
        compiler_params=pltpu.CompilerParams(
            collective_id=0, has_side_effects=True, vmem_limit_bytes=61 * 2**20
        ),
        name="layer",
    )(
        tokens.reshape(length, model), first_gain[None], in_matrix, in_scale[None], conv_taps, decay_rate,
        recall_maps, admit_maps, out_matrix, second_gain[None], up_matrix, up_scale[None], down_matrix,
        jnp.stack([out_scale, down_scale]),
    )
    return result.reshape(tokens.shape)


def solution(mesh):
    placed = (
        P(("rep", "fs"), None, None),
        P(),
        P("fs", "tp"),
        P("tp"),
        P(None, "tp"),
        P(None, "tp"),
        P(None, "tp", None, None),
        P(None, "tp", None, None),
        P("fs", "tp"),
        P("fs"),
        P(),
        P("fs", "tp"),
        P("tp"),
        P("fs", "tp"),
        P("fs"),
    )
    small = (mesh.shape["rep"], mesh.shape["fs"], mesh.shape["tp"]) == (2, 4, 4)
    return jax.shard_map(
        fused_body if small else body, mesh=mesh, in_specs=placed, out_specs=P(("rep", "fs"), None, None), check_vma=False
    )
```

```python
import functools
import jax
import jax.numpy as jnp
from jax import lax
from jax.experimental import pallas as pl
from jax.experimental.pallas import tpu as pltpu
from jax.sharding import PartitionSpec as P

EPSILON = 1e-06
RATE_GAIN = 8.0
LANES = 128
SEGMENTS = 8
PAD = 8


def normalize(stream, gain):
    return stream * lax.rsqrt(jnp.mean(stream * stream, axis=-1, keepdims=True) + EPSILON) * gain


def one_minus_exp(y):
    series = 1.0 + y * (1.0 / 6.0)
    for k in (5.0, 4.0, 3.0, 2.0):
        series = 1.0 + y * (1.0 / k) * series
    return jnp.where(y > -0.25, -y * series, 1.0 - jnp.exp(y))


def sigmoid(x):
    return 0.5 * jnp.tanh(0.5 * x) + 0.5


def gate_part(padded, taps_ref, rate_ref, recall_ref, admit_ref, decay, drive, length):
    directions, groups, block, _ = recall_ref.shape
    taps = taps_ref.shape[0]
    rows = length // SEGMENTS

    def tile_step(tile, _):
        base = pl.multiple_of(tile * rows, rows)
        conv = jnp.zeros((rows, padded.shape[1]), jnp.float32)
        window = padded[pl.ds(base, rows + 2 * PAD), :]
        for k in range(taps):
            first = PAD - taps // 2 + k
            conv = conv + taps_ref[k : k + 1, :] * window[first : first + rows, :]
        narrow = conv.astype(jnp.bfloat16)
        for g in range(groups):
            values = conv[:, g * block : (g + 1) * block]
            left = narrow[:, g * block : (g + 1) * block]
            for d in range(directions):
                recall = sigmoid(jnp.dot(left, recall_ref[d, g].astype(jnp.bfloat16), preferred_element_type=jnp.float32))
                admit = sigmoid(jnp.dot(left, admit_ref[d, g].astype(jnp.bfloat16), preferred_element_type=jnp.float32))
                log_decay = recall * (-RATE_GAIN * rate_ref[d : d + 1, g * block : (g + 1) * block])
                a = jnp.exp(log_decay)
                b = jnp.sqrt(one_minus_exp(2.0 * log_decay)) * admit * values
                for c in range(block // LANES):
                    where = g * (block // LANES) + c
                    decay[d, where, pl.ds(base, rows), :] = a[:, c * LANES : (c + 1) * LANES]
                    drive[d, where, pl.ds(base, rows), :] = b[:, c * LANES : (c + 1) * LANES]
        return 0

    lax.fori_loop(0, SEGMENTS, tile_step, 0)


def scan_part(decay, drive, prefix, mixed_ref, length):
    directions, chunks = decay.shape[:2]
    steps = length // SEGMENTS
    lanes = [(d, c) for d in range(directions) for c in range(chunks)]

    def scan_step(s, carried):
        out = []
        for (d, c), (state, product) in zip(lanes, carried):
            at = s if d == 0 else steps - 1 - s
            a = decay[d, c, pl.ds(at, SEGMENTS, stride=steps), :]
            b = drive[d, c, pl.ds(at, SEGMENTS, stride=steps), :]
            state = a * state + b
            product = a * product
            drive[d, c, pl.ds(at, SEGMENTS, stride=steps), :] = state
            prefix[d, c, pl.ds(at, SEGMENTS, stride=steps), :] = product
            out.append((state, product))
        return tuple(out)

    start = tuple((jnp.zeros((SEGMENTS, LANES), jnp.float32), jnp.ones((SEGMENTS, LANES), jnp.float32)) for _ in lanes)
    ends = lax.fori_loop(0, steps, scan_step, start, unroll=4)
    ends = dict(zip(lanes, ends))

    for c in range(chunks):
        carries = []
        for d in range(directions):
            state, product = ends[(d, c)]
            order = range(SEGMENTS) if d == 0 else range(SEGMENTS - 1, -1, -1)
            carry = jnp.zeros((1, LANES), jnp.float32)
            entering = {}
            for k in order:
                entering[k] = carry
                carry = product[k : k + 1, :] * carry + state[k : k + 1, :]
            carries.append(entering)
        for k in range(SEGMENTS):
            span = pl.ds(k * steps, steps)
            total = drive[0, c, span, :] + prefix[0, c, span, :] * carries[0][k]
            total = total + (drive[1, c, span, :] + prefix[1, c, span, :] * carries[1][k])
            mixed_ref[span, c * LANES : (c + 1) * LANES] = total.astype(jnp.bfloat16)


def recurrence_kernel(before_ref, taps_ref, rate_ref, recall_ref, admit_ref, mixed_ref, padded, decay, drive, prefix):
    length, width = before_ref.shape
    edge = jnp.zeros((PAD, width), jnp.float32)
    padded[pl.ds(0, PAD), :] = edge
    padded[pl.ds(PAD + length, PAD), :] = edge
    padded[pl.ds(PAD, length), :] = before_ref[...].astype(jnp.float32)
    gate_part(padded, taps_ref, rate_ref, recall_ref, admit_ref, decay, drive, length)
    scan_part(decay, drive, prefix, mixed_ref, length)


def recurrence(before, taps, rates, recall_maps, admit_maps):
    length, width = before.shape
    directions = rates.shape[0]
    chunks = width // LANES
    plane = pltpu.VMEM((directions, chunks, length, LANES), jnp.float32)
    return pl.pallas_call(
        recurrence_kernel,
        out_shape=jax.ShapeDtypeStruct((length, width), jnp.bfloat16),
        in_specs=[pl.BlockSpec(memory_space=pltpu.VMEM)] * 5,
        out_specs=pl.BlockSpec(memory_space=pltpu.VMEM),
        scratch_shapes=[pltpu.VMEM((length + 2 * PAD, width), jnp.float32), plane, plane, plane],
        compiler_params=pltpu.CompilerParams(vmem_limit_bytes=24 * 2**20),
        cost_estimate=pl.CostEstimate(flops=16 * length * width * 256, bytes_accessed=8 * 2**20, transcendentals=8 * length * width),
        name="recurrence",
    )(before, taps, rates, recall_maps, admit_maps)


def contract_last(left, right):
    return lax.dot_general(
        left, right, (((1,), (1,)), ((), ())), preferred_element_type=jnp.float32
    )


def gather(shard):
    copies = lax.axis_size("rep")
    if shard.shape[0] % (16 * copies):
        return lax.all_gather(shard.astype(jnp.bfloat16), "fs", axis=0, tiled=True)
    rows = shard.shape[0] // copies
    part = lax.dynamic_slice_in_dim(shard, lax.axis_index("rep") * rows, rows, 0)
    return lax.all_gather(part.astype(jnp.bfloat16), ("fs", "rep"), axis=0, tiled=True)


def body(
    tokens,
    first_gain,
    in_matrix,
    in_scale,
    conv_taps,
    decay_rate,
    recall_maps,
    admit_maps,
    out_matrix,
    out_scale,
    second_gain,
    up_matrix,
    up_scale,
    down_matrix,
    down_scale,
):
    stream = tokens.reshape(tokens.shape[1], tokens.shape[2]).astype(jnp.float32)
    factors = lax.all_gather(
        jnp.stack([out_scale, down_scale]).astype(jnp.bfloat16), "fs", axis=1, tiled=True
    )
    in_cols = gather(in_matrix)
    normed = normalize(stream, first_gain).astype(jnp.bfloat16)
    before = (
        jnp.dot(normed, in_cols, preferred_element_type=jnp.float32) * in_scale.astype(jnp.bfloat16)
    ).astype(jnp.bfloat16)
    mixed = recurrence(before, conv_taps, decay_rate, recall_maps, admit_maps)
    partial_value = contract_last(mixed, gather(out_matrix))
    middle = stream + factors[0] * lax.psum(partial_value.astype(jnp.bfloat16), "tp").astype(
        jnp.float32
    )
    second_normed = normalize(middle, second_gain).astype(jnp.bfloat16)
    raised = jnp.dot(second_normed, gather(up_matrix), preferred_element_type=jnp.float32)
    active = jnp.square(jax.nn.relu(raised * up_scale.astype(jnp.bfloat16))).astype(jnp.bfloat16)
    lowered = contract_last(active, gather(down_matrix))
    result = (
        middle + factors[1] * lax.psum(lowered.astype(jnp.bfloat16), "tp").astype(jnp.float32)
    ).astype(jnp.bfloat16)
    return result.reshape(tokens.shape)

MESH = pl.DeviceIdType.MESH


def layer_kernel(
    names, tokens_ref, first_ref, in_ref, in_scale_ref, taps_ref, rate_ref, recall_ref, admit_ref,
    out_ref, second_ref, up_ref, up_scale_ref, down_ref, scales_ref,
    result_ref,
    in_all, out_all, up_all, down_all, scales_all, normed, padded, decay, drive, prefix, mixed, active,
    first_parts, first_sums, second_parts, second_sums, middle, send, recv,
):
    replica, place, rank = (lax.axis_index(name) for name in names)
    rep_name, fs_name, tp_name = names
    fs, tp = 4, 4
    length, model = tokens_ref.shape
    rows = length // tp
    block = model // fs
    right, left, across = (lax.rem(place + k, fs) for k in (1, 3, 2))
    mate = 1 - replica
    near = rank + 1 - 2 * lax.rem(rank, 2)
    far = lax.rem(rank + 2, tp)
    count = [0]

    def copy(src, dst, axis, peer):
        index = count[0]
        count[0] += 1
        return pltpu.make_async_remote_copy(
            src_ref=src, dst_ref=dst, send_sem=send.at[index], recv_sem=recv.at[index],
            device_id={axis: peer}, device_id_type=MESH,
        )

    started = []

    def start(*copies):
        for one in copies:
            one.start()
            started.append(one)

    class Gather:
        def __init__(self, whole):
            def view(owner, offset, size):
                return whole.at[pl.ds(pl.multiple_of(owner * block + replica * half + offset, quarter), size), :]

            half, quarter = block // 2, block // 4
            own = view(place, 0, half)
            from_left, from_right = view(left, 0, half), view(right, 0, half)
            self.to_right = copy(own, own, fs_name, right)
            self.to_left = copy(own, own, fs_name, left)
            low, high = view(left, 0, quarter), view(right, quarter, quarter)
            self.on_right = copy(low, low, fs_name, right)
            self.on_left = copy(high, high, fs_name, left)
            opposite = view(across, 0, half)
            self.swaps = [copy(part, part, rep_name, mate) for part in (from_left, from_right, opposite)]

        def first(self):
            start(self.to_right, self.to_left)

        def second(self):
            self.to_right.wait_recv()
            start(self.on_right, self.swaps[0])
            self.to_left.wait_recv()
            start(self.on_left, self.swaps[1])

        def third(self):
            self.on_right.wait_recv()
            self.on_left.wait_recv()
            start(self.swaps[2])

        def finish(self):
            for swap in self.swaps:
                swap.wait_recv()

    barrier = pltpu.get_barrier_semaphore()
    greeted = [(rep_name, mate), (fs_name, right), (fs_name, left), (fs_name, across)]
    greeted += [(tp_name, lax.rem(rank + k, tp)) for k in range(1, tp)]
    for axis, peer in greeted:
        pl.semaphore_signal(barrier, inc=1, device_id={axis: peer}, device_id_type=MESH)

    own_rows = pl.ds(pl.multiple_of(place * block, block), block)
    for shard, whole in ((in_ref, in_all), (out_ref, out_all), (up_ref, up_all), (down_ref, down_all)):
        whole[own_rows, :] = shard[...].astype(jnp.bfloat16)
    scales_all[place] = scales_ref[...]
    pl.semaphore_wait(barrier, len(greeted))

    g_in, g_out, g_up, g_down = (Gather(whole) for whole in (in_all, out_all, up_all, down_all))
    g_in.first()
    scale_copies = [
        copy(scales_ref, scales_all.at[place], fs_name, lax.rem(place + k, fs)) for k in range(1, fs)
    ]
    start(*scale_copies)
    g_out.first()

    tile = 64

    def norm_step(i, _):
        at = pl.ds(pl.multiple_of(i * tile, tile), tile)
        normed[at, :] = normalize(tokens_ref[at, :].astype(jnp.float32), first_ref[...]).astype(jnp.bfloat16)
        return 0

    lax.fori_loop(0, length // tile, norm_step, 0)

    g_in.second()
    g_in.third()
    g_out.second()
    g_up.first()
    g_in.finish()

    edge = jnp.zeros((PAD, padded.shape[1]), jnp.float32)
    padded[pl.ds(0, PAD), :] = edge
    padded[pl.ds(PAD + length, PAD), :] = edge
    wide = 256

    def in_step(i, _):
        at = pl.ds(pl.multiple_of(i * wide, wide), wide)
        product = jnp.dot(normed[...], in_all[:, at], preferred_element_type=jnp.float32)
        product = product * in_scale_ref[:, at].astype(jnp.bfloat16).astype(jnp.float32)
        padded[pl.ds(PAD, length), at] = product.astype(jnp.bfloat16).astype(jnp.float32)
        return 0

    lax.fori_loop(0, in_all.shape[1] // wide, in_step, 0)
    g_out.third()
    gate_part(padded, taps_ref, rate_ref, recall_ref, admit_ref, decay, drive, length)
    g_up.second()
    g_down.first()
    scan_part(decay, drive, prefix, mixed, length)
    g_up.third()
    for one in scale_copies:
        one.wait_recv()

    order = (place, left, right, across)

    def project(gathered, values, whole, parts, sums, between):
        hops = []

        def send_block(j):
            hop = []
            for k in range(1, tp):
                peer = lax.rem(rank + k, tp)
                hop.append(copy(parts.at[j, pl.ds(pl.multiple_of(peer * rows, rows), rows), :], sums.at[k - 1, j], tp_name, peer))
            start(*hop)
            hops.append(hop)

        for j in range(fs):
            if j:
                gathered.swaps[j - 1].wait_recv()

            def step(i, _):
                at = pl.ds(pl.multiple_of(i * wide, wide), wide)
                matrix = whole[pl.ds(pl.multiple_of(order[j] * block + i * wide, wide), wide), :]
                parts[j, :, at] = contract_last(values[...], matrix).astype(jnp.bfloat16)
                return 0

            lax.fori_loop(0, block // wide, step, 0)
            if j:
                send_block(j - 1)
            between(j)
        send_block(fs - 1)
        return hops

    own_quarter = pl.ds(pl.multiple_of(rank * rows, rows), rows)

    def summed(parts, sums, hops, j):
        for hop in hops[j]:
            hop.wait_recv()
        total = parts[j, own_quarter, :].astype(jnp.float32)
        for k in range(tp - 1):
            total = total + sums[k, j].astype(jnp.float32)
        return total

    def factor(j, which):
        return scales_all[order[j], which : which + 1, :].astype(jnp.bfloat16).astype(jnp.float32)

    def advance(j):
        if j == 1:
            g_down.second()

    hops = project(g_out, mixed, out_all, first_parts, first_sums, advance)
    squares = jnp.zeros((rows, 1), jnp.float32)
    for j in range(fs):
        columns = pl.ds(pl.multiple_of(order[j] * block, block), block)
        value = tokens_ref[own_quarter, columns].astype(jnp.float32) + factor(j, 0) * summed(first_parts, first_sums, hops, j)
        middle[:, columns] = value
        squares = squares + jnp.sum(value * value, axis=1, keepdims=True)
    inverse = lax.rsqrt(squares * (1.0 / model) + EPSILON)
    normed[own_quarter, :] = (middle[...] * inverse * second_ref[...]).astype(jnp.bfloat16)

    def spread(ref, columns):
        own = ref.at[own_quarter, columns]
        theirs = ref.at[pl.ds(pl.multiple_of(far * rows, rows), rows), columns]
        return copy(own, own, tp_name, far), copy(own, own, tp_name, near), copy(theirs, theirs, tp_name, near)

    whole_width = pl.ds(0, model)
    to_far, to_near, onward = spread(normed, whole_width)
    g_up.swaps[0].wait_recv()
    start(to_far, to_near)
    to_far.wait_recv()
    start(onward)
    g_down.third()
    g_up.swaps[1].wait_recv()
    g_up.swaps[2].wait_recv()
    to_near.wait_recv()
    onward.wait_recv()

    def up_step(i, _):
        at = pl.ds(pl.multiple_of(i * wide, wide), wide)
        raised = jnp.dot(normed[...], up_all[:, at], preferred_element_type=jnp.float32)
        raised = raised * up_scale_ref[:, at].astype(jnp.bfloat16).astype(jnp.float32)
        active[:, at] = jnp.square(jnp.maximum(raised, 0.0)).astype(jnp.bfloat16)
        return 0

    lax.fori_loop(0, up_all.shape[1] // wide, up_step, 0)
    hops = project(g_down, active, down_all, second_parts, second_sums, lambda j: None)
    spreads = []
    for j in range(fs):
        columns = pl.ds(pl.multiple_of(order[j] * block, block), block)
        value = middle[:, columns] + factor(j, 1) * summed(second_parts, second_sums, hops, j)
        result_ref[own_quarter, columns] = value.astype(jnp.bfloat16)
        spreads.append(spread(result_ref, columns))
        start(*spreads[j][:2])
        if j:
            spreads[j - 1][0].wait_recv()
            start(spreads[j - 1][2])
    spreads[-1][0].wait_recv()
    start(spreads[-1][2])
    for _, to_near, onward in spreads:
        to_near.wait_recv()
        onward.wait_recv()
    for one in started:
        one.wait_send()


def fused_body(
    tokens, first_gain, in_matrix, in_scale, conv_taps, decay_rate, recall_maps, admit_maps,
    out_matrix, out_scale, second_gain, up_matrix, up_scale, down_matrix, down_scale,
):
    length, model = tokens.shape[1:]
    width, hidden = in_matrix.shape[1], up_matrix.shape[1]
    fs, tp = lax.axis_size("fs"), lax.axis_size("tp")
    rows, block = length // tp, model // fs
    directions = decay_rate.shape[0]
    plane = pltpu.VMEM((directions, width // LANES, length, LANES), jnp.float32)
    parts = pltpu.VMEM((fs, length, block), jnp.bfloat16)
    sums = pltpu.VMEM((tp - 1, fs, rows, block), jnp.bfloat16)
    copies = 4 * 7 + 3 + 2 * 12 + 3 + 12
    result = pl.pallas_call(
        functools.partial(layer_kernel, ("rep", "fs", "tp")),
        out_shape=jax.ShapeDtypeStruct((length, model), jnp.bfloat16),
        in_specs=[pl.BlockSpec(memory_space=pltpu.VMEM)] * 14,
        out_specs=pl.BlockSpec(memory_space=pltpu.VMEM),
        scratch_shapes=[
            pltpu.VMEM((model, width), jnp.bfloat16),
            pltpu.VMEM((model, width), jnp.bfloat16),
            pltpu.VMEM((model, hidden), jnp.bfloat16),
            pltpu.VMEM((model, hidden), jnp.bfloat16),
            pltpu.VMEM((fs, 2, block), jnp.float32),
            pltpu.VMEM((length, model), jnp.bfloat16),
            pltpu.VMEM((length + 2 * PAD, width), jnp.float32),
            plane, plane, plane,
            pltpu.VMEM((length, width), jnp.bfloat16),
            pltpu.VMEM((length, hidden), jnp.bfloat16),
            parts, sums, parts, sums,
            pltpu.VMEM((rows, model), jnp.float32),
            pltpu.SemaphoreType.DMA((copies,)),
            pltpu.SemaphoreType.DMA((copies,)),
        ],
        compiler_params=pltpu.CompilerParams(
            collective_id=0, has_side_effects=True, vmem_limit_bytes=61 * 2**20
        ),
        name="layer",
    )(
        tokens.reshape(length, model), first_gain[None], in_matrix, in_scale[None], conv_taps, decay_rate,
        recall_maps, admit_maps, out_matrix, second_gain[None], up_matrix, up_scale[None], down_matrix,
        jnp.stack([out_scale, down_scale]),
    )
    return result.reshape(tokens.shape)


def solution(mesh):
    placed = (
        P(("rep", "fs"), None, None),
        P(),
        P("fs", "tp"),
        P("tp"),
        P(None, "tp"),
        P(None, "tp"),
        P(None, "tp", None, None),
        P(None, "tp", None, None),
        P("fs", "tp"),
        P("fs"),
        P(),
        P("fs", "tp"),
        P("tp"),
        P("fs", "tp"),
        P("fs"),
    )
    small = (mesh.shape["rep"], mesh.shape["fs"], mesh.shape["tp"]) == (2, 4, 4)
    return jax.shard_map(
        fused_body if small else body, mesh=mesh, in_specs=placed, out_specs=P(("rep", "fs"), None, None), check_vma=False
    )
```
